128 devices in a mesh: ep: 32 (over z, y, core), tp: 4 (over x).
Axes of the slice: x: 4, y: 4, z: 4, core: 2. Of those that a mesh axis runs over, the one named last changes fastest.
Arguments:
- x_mix: bfloat16 [32768, 2048], P('ep'), may hold values from -6 to 6
- mix_gain: float32 [2048], replicated, may hold values from 0.1 to 1.9
- w_query: bfloat16 [2048, 1024], P(None, 'tp'), may hold values from -0.125 to 0.125
- w_key: bfloat16 [2048, 1024], P(None, 'tp'), may hold values from -0.125 to 0.125
- w_value: bfloat16 [2048, 1024], P(None, 'tp'), may hold values from -0.125 to 0.125
- w_outgate: bfloat16 [2048, 1024], P(None, 'tp'), may hold values from -0.125 to 0.125
- w_gates: bfloat16 [2048, 32], replicated, may hold values from -0.125 to 0.125
- gate_bias: float32 [4, 8], P(None, 'tp'), may hold values from -1 to 120, as said below
- gate_drift: float32 [128], P('ep'), may hold values from -1.5 to 1.5
- head_gain: float32 [1024], P('tp'), may hold values from 0.1 to 1.9
- w_out: bfloat16 [1024, 2048], P('tp'), may hold values from -0.1875 to 0.1875
- x_route: bfloat16 [16384, 2048], P('ep'), may hold values from -6 to 6
- route_gain: float32 [2048], replicated, may hold values from 0.1 to 1.9
- routes: int32 [16384, 2], P('ep'), may hold values from 0 to 31, all different within a row; in each aligned block of 128 rows (0 to 127, 128 to 255, ...) at most 16 rows name the same one
- route_weight: float32 [16384, 2], P(('ep', 'tp')), may hold values from 0.2 to 1
- w_gate_e: bfloat16 [32, 2048, 1024], P('ep', None, 'tp'), may hold values from -0.125 to 0.125
- w_up_e: bfloat16 [32, 2048, 1024], P('ep', None, 'tp'), may hold values from -0.125 to 0.125
- w_down_e: bfloat16 [32, 1024, 2048], P('ep', 'tp'), may hold values from -0.1875 to 0.1875
Outputs:
- mixer_out: bfloat16 [32768, 2048], P(('ep', 'tp'))
- route_out: bfloat16 [16384, 2048], P(('ep', 'tp'))
The draws below stay inside these ranges and needn't reach their ends.
Inputs may be any that keep to these rules, and one draw needn't show every extreme that they name: `routes`: in each aligned block of 128 rows, no expert is named by more than 16 entries; the 2 experts of a row differ. `gate_bias`: rows 0 and 2 are input gate offsets, rows 1 and 3 forget gate offsets.
All inputs are finite; a program needn't handle non-finite values.
Results may differ from the reference program's by a relative error of at most 0.017.
Values may be sent and summed in bfloat16 or wider, within the bound.
A program may use at most 128 MiB of HBM per device.

```python
import math
import jax
import jax.numpy as jnp
import numpy as np
from jax import lax

D = 2048
HM = 8
HD = 128
FE = 1024
TOPK = 2
BLK = 256
EXPERTS = 32
TOKENS_A = 32768
TOKENS_B = 16384
QROWS = 128
CAPQ = 16
N_TP = 4


def draw_gate_bias(key, part):
    subkeys = jax.random.split(jax.random.fold_in(key, 17), 4)
    inputs = jax.random.uniform(subkeys[0], (2, HM), jnp.float32, -1.0, 1.0)
    slow_heads = jax.random.bernoulli(subkeys[1], 0.5, (2, HM))
    fast_values = jax.random.uniform(subkeys[2], (2, HM), jnp.float32, 4.0, 5.0)
    slow_values = jax.random.uniform(subkeys[3], (2, HM), jnp.float32, 11.0, 12.5)
    forget = jnp.where(slow_heads, slow_values, fast_values)
    return jnp.stack([inputs[0], forget[0], inputs[1], forget[1]], axis=0)


def steps_of(own_key, shape, cuts, smallest, top_value):
    def one(dim, parts):
        steps = jax.random.uniform(jax.random.fold_in(jax.random.fold_in(own_key, 6), dim), (parts,), jnp.float32, smallest / len(cuts), top_value / len(cuts))
        return jnp.repeat(jnp.exp(steps), shape[dim] // parts).reshape((-1,) + (1,) * (len(shape) - dim - 1))

    level = one(*cuts[0])
    for cut in cuts[1:]:
        level = level * one(*cut)
    return level


def routed_block(rng, own, number, rows, count, top, bound, skew):
    order = jax.random.permutation(rng, count)
    crowded, usual = load_shares(count, rows * top, bound, skew, True), load_shares(count, rows * top, bound, skew, False)
    places = jnp.arange(count)

    def named(lengths, turn):
        used = int((lengths > 0).sum())
        fixed = max(1, used // 4)
        moved = fixed + (places - fixed + turn * (used - fixed)) % max(1, count - fixed)
        return jnp.zeros((count,), jnp.int32).at[order[jnp.where(places < fixed, places, moved)]].set(jnp.asarray(lengths, jnp.int32))

    lengths = jnp.where(number % 4 == 0, named(crowded, number // 4), named(usual, number - number // 4 - 1))
    mixed = jax.random.permutation(jax.random.fold_in(own, 3), count)
    donor, taker = mixed[0:count // 2 * 2:2], mixed[1:count // 2 * 2:2]
    margin = jnp.minimum(lengths[donor] - 1, bound - lengths[taker]) // 2
    margin = jnp.where((donor == order[0]) | (taker == order[0]) | (lengths[taker] == 0), 0, jnp.maximum(margin, 0))
    moved = jax.random.randint(jax.random.fold_in(own, 4), (count // 2,), 0, 1 << 20) % (margin + 1)
    lengths = lengths.at[donor].add(-moved).at[taker].add(moved)
    members = jnp.searchsorted(jnp.cumsum(lengths), jnp.arange(rows * top), side="right").astype(jnp.int32)
    table = members.reshape(top, rows).T
    table = table[jax.random.permutation(jax.random.fold_in(own, 1), rows)]
    turn = jax.random.randint(jax.random.fold_in(own, 2), (rows, 1), 0, top)
    return jnp.take_along_axis(table, (jnp.arange(top)[None, :] + turn) % top, axis=1)


def load_shares(amount, total, most, skew, full):
    weights = [(1 << 20) // math.isqrt(rank ** skew) + 1 for rank in range(1, amount + 1)]
    largest = most if full else min(most, max(-(-total // amount), total * weights[0] // sum(weights)))
    least = 1 if total - largest >= amount - 1 else 0
    given, surplus = [largest] + [least] * (amount - 1), total - largest - least * (amount - 1)
    while surplus > 0:
        movable = [i for i in range(1, amount) if given[i] < largest] or [i for i in range(1, amount) if given[i] < most]
        pool, remaining = sum([weights[i] for i in movable]), surplus
        for i in movable:
            extra = min(most - given[i], max(1, remaining * weights[i] // pool), surplus)
            given[i] = given[i] + extra
            surplus = surplus - extra
    return np.array(given)


def noise(own_key, dims, deviation, bound, cuts=(), kind=jnp.bfloat16):
    array = jax.random.normal(own_key, dims, jnp.float32) * deviation
    if len(cuts) > 0:
        array = steps_of(own_key, dims, cuts, -0.22, 0.18) * array
    return jnp.clip(array, min=-bound, max=bound).astype(kind)


def setup_inputs(seed: int = 0) -> dict:
    seeds = jax.random.split(jax.random.key(seed), 19)
    x_mix = noise(seeds[0], (TOKENS_A, D), 1.0, 6.0, ((0, 32),))
    mix_gain = jnp.clip(1.0 + 0.18 * jax.random.normal(seeds[1], (D,), jnp.float32), 0.1, 1.9)
    w_query = noise(seeds[2], (D, HM * HD), D ** -0.5, 0.125, ((1, 4),))
    w_key = noise(seeds[3], (D, HM * HD), D ** -0.5, 0.125, ((1, 4),))
    w_value = noise(seeds[4], (D, HM * HD), D ** -0.5, 0.125, ((1, 4),))
    w_outgate = noise(seeds[5], (D, HM * HD), D ** -0.5, 0.125, ((1, 4),))
    w_gates = noise(seeds[6], (D, 4 * HM), D ** -0.5, 0.125)
    gate_bias = draw_gate_bias(jax.random.fold_in(seeds[18], 71), 0)
    gate_drift = jnp.clip(jax.random.uniform(seeds[8], (TOKENS_A // BLK,), jnp.float32, -1.5, 1.5) * steps_of(seeds[8], (TOKENS_A // BLK,), ((0, 32),), -0.4, 0.0), -1.5, 1.5)
    head_gain = jnp.clip(1.0 + 0.18 * jax.random.normal(seeds[9], (HM * HD,), jnp.float32), 0.1, 1.9)
    w_out = noise(seeds[10], (HM * HD, D), (HM * HD) ** -0.5, 0.1875, ((0, 4),))
    x_route = noise(seeds[11], (TOKENS_B, D), 1.0, 6.0, ((0, 32),))
    route_gain = jnp.clip(1.0 + 0.18 * jax.random.normal(seeds[12], (D,), jnp.float32), 0.1, 1.9)
    routes_keys = jax.random.split(jax.random.fold_in(seeds[13], 1), TOKENS_B // QROWS)
    routes_turns = jax.random.permutation(jax.random.fold_in(seeds[13], 3), TOKENS_B // QROWS)
    routes = jax.vmap(lambda own, number: routed_block(jax.random.fold_in(seeds[13], 2), own, number, QROWS, EXPERTS, TOPK, CAPQ, 2))(routes_keys, routes_turns).reshape((TOKENS_B, TOPK))
    route_weight = jnp.clip(0.2 + 0.8 * jax.random.uniform(seeds[14], (TOKENS_B, TOPK), jnp.float32) ** steps_of(seeds[14], (TOKENS_B, TOPK), ((0, 128),), -0.2, 0.2), 0.2, 1.0)
    w_gate_e = noise(seeds[15], (EXPERTS, D, FE), D ** -0.5, 0.125, ((0, 32), (2, 4)))
    w_up_e = noise(seeds[16], (EXPERTS, D, FE), D ** -0.5, 0.125, ((0, 32), (2, 4)))
    w_down_e = noise(seeds[17], (EXPERTS, FE, D), FE ** -0.5, 0.1875, ((0, 32), (1, 4)))
    return {"x_mix": x_mix, "mix_gain": mix_gain, "w_query": w_query, "w_key": w_key, "w_value": w_value, "w_outgate": w_outgate, "w_gates": w_gates, "gate_bias": gate_bias, "gate_drift": gate_drift, "head_gain": head_gain, "w_out": w_out, "x_route": x_route, "route_gain": route_gain, "routes": routes, "route_weight": route_weight, "w_gate_e": w_gate_e, "w_up_e": w_up_e, "w_down_e": w_down_e}


EPS = 1e-06
NEG = -1e+30
HIGH = lax.Precision.HIGHEST

def rms_scale(tensor, gain):
    tensor = tensor.astype(jnp.float32)
    return tensor * lax.rsqrt(lax.optimization_barrier(jnp.mean(tensor * tensor, axis=-1, keepdims=True)) + EPS) * gain.astype(jnp.float32)

def run_blocks(query, key_rows, value_rows, log_input, log_forget, state_in):
    head_count, row_count, head_width = query.shape
    block_count = row_count // BLK

    def in_blocks(tensor):
        return jnp.moveaxis(tensor.reshape((head_count, block_count, BLK) + tensor.shape[2:]), 1, 0)
    tri_mask = jnp.tril(jnp.ones((BLK, BLK), dtype=bool))

    def advance(state_now, pieces):
        memory, normer, stable = state_now
        q_block, k_block, v_block, in_block, forget_block = pieces
        q_wide = q_block.astype(jnp.float32)
        k_wide = k_block.astype(jnp.float32)
        v_wide = v_block.astype(jnp.float32)
        running = jnp.cumsum(forget_block, axis=-1)
        log_decay = jnp.where(tri_mask, running[:, :, None] - running[:, None, :] + in_block[:, None, :], NEG)
        carried = running + stable[:, None]
        stable_t = jnp.maximum(carried, lax.optimization_barrier(jnp.max(log_decay, axis=-1)))
        raw = jnp.einsum('htd,hsd->hts', q_block, k_block, preferred_element_type=jnp.float32)
        scores = raw * jnp.exp(log_decay - stable_t[:, :, None])
        carried_w = jnp.exp(carried - stable_t)
        numerator = jnp.einsum('hts,hse->hte', scores, v_wide, precision=HIGH) + carried_w[:, :, None] * jnp.einsum('htd,hde->hte', q_wide, memory, precision=HIGH)
        denominator = lax.optimization_barrier(jnp.sum(scores, axis=-1)) + carried_w * jnp.einsum('htd,hd->ht', q_wide, normer, precision=HIGH)
        result = numerator / jnp.maximum(jnp.abs(denominator), jnp.exp(-stable_t))[:, :, None]
        block_total = running[:, -1]
        log_weight = block_total[:, None] - running + in_block
        stable_new = jnp.maximum(block_total + stable, lax.optimization_barrier(jnp.max(log_weight, axis=-1)))
        weights = jnp.exp(log_weight - stable_new[:, None])
        shrink = jnp.exp(block_total + stable - stable_new)
        memory = shrink[:, None, None] * memory + jnp.einsum('hs,hsd,hse->hde', weights, k_wide, v_wide, precision=HIGH)
        normer = shrink[:, None] * normer + jnp.einsum('hs,hsd->hd', weights, k_wide, precision=HIGH)
        return ((memory, normer, stable_new), result)
    final_state, outputs = lax.scan(advance, state_in, tuple((in_blocks(t) for t in (query, key_rows, value_rows, log_input, log_forget))))
    return jnp.moveaxis(outputs, 0, 1).reshape(head_count, row_count, head_width)

def reverse_rows(tensor):
    return jnp.flip(tensor, axis=1)

def group_sum(left, right, groups):
    part_size = left.shape[1] // groups
    total = jnp.zeros((left.shape[0], right.shape[1]), jnp.float32)
    for group in range(groups):
        piece = jnp.dot(left[:, group * part_size:(group + 1) * part_size], right[group * part_size:(group + 1) * part_size], preferred_element_type=jnp.float32)
        total = total + lax.optimization_barrier(piece.astype(jnp.bfloat16)).astype(jnp.float32)
    return total.astype(jnp.bfloat16)

def reference(x_mix, mix_gain, w_query, w_key, w_value, w_outgate, w_gates, gate_bias, gate_drift, head_gain, w_out, x_route, route_gain, routes, route_weight, w_gate_e, w_up_e, w_down_e):
    seq_len = x_mix.shape[0]
    normed = rms_scale(x_mix, mix_gain).astype(jnp.bfloat16)
    query = jnp.dot(normed, w_query, preferred_element_type=jnp.float32).astype(jnp.bfloat16)
    key_rows = (jnp.dot(normed, w_key, preferred_element_type=jnp.float32) * HD ** (-0.5)).astype(jnp.bfloat16)
    value_rows = jnp.dot(normed, w_value, preferred_element_type=jnp.float32).astype(jnp.bfloat16)
    outgate = jnp.dot(normed, w_outgate, preferred_element_type=jnp.float32).astype(jnp.bfloat16)
    gate_pre = jnp.dot(normed, w_gates, preferred_element_type=jnp.float32).reshape(seq_len, 4, HM) + gate_bias[None]
    drift = jnp.repeat(gate_drift, BLK)[:, None]
    in_fw = gate_pre[:, 0].T
    forget_fw = jax.nn.log_sigmoid(gate_pre[:, 1] + drift).T
    in_bw = gate_pre[:, 2].T
    forget_bw = jax.nn.log_sigmoid(gate_pre[:, 3] + drift).T

    def heads_first(tensor):
        return tensor.reshape(seq_len, HM, HD).transpose(1, 0, 2)

    def one_head(pieces):
        q_head, k_head, v_head, in_f, forget_f, in_b, forget_b = pieces
        start = (jnp.zeros((1, HD, HD), jnp.float32), jnp.zeros((1, HD), jnp.float32), jnp.zeros((1,), jnp.float32))
        forward = run_blocks(q_head[None], k_head[None], v_head[None], in_f[None], forget_f[None], start)
        backward = reverse_rows(run_blocks(reverse_rows(q_head[None]), reverse_rows(k_head[None]), reverse_rows(v_head[None]), reverse_rows(in_b[None]), reverse_rows(forget_b[None]), start))
        return (forward + backward)[0]
    mixed = lax.map(one_head, (heads_first(query), heads_first(key_rows), heads_first(value_rows), in_fw, forget_fw, in_bw, forget_bw))
    mixed = mixed.transpose(1, 0, 2)
    gated = jax.nn.sigmoid(outgate.astype(jnp.float32)).reshape(seq_len, HM, HD) * mixed
    head_rows = rms_scale(gated, head_gain.reshape(HM, HD)).astype(jnp.bfloat16).reshape(seq_len, HM * HD)
    mixer_out = group_sum(head_rows, w_out, N_TP)
    token_count = x_route.shape[0]
    route_normed = rms_scale(x_route, route_gain).astype(jnp.bfloat16)
    block_total = token_count // QROWS
    flat_routes = routes.reshape(block_total, QROWS * TOPK)
    onehot = (flat_routes[:, :, None] == jnp.arange(EXPERTS, dtype=jnp.int32)[None, None, :]).astype(jnp.int32)
    ranks = lax.optimization_barrier(jnp.sum((jnp.cumsum(onehot, axis=1) - onehot) * onehot, axis=2))
    per_expert = block_total * CAPQ
    slots = (flat_routes * per_expert + jnp.arange(block_total, dtype=jnp.int32)[:, None] * CAPQ + ranks).reshape(-1).astype(jnp.int32)
    token_ids = jnp.repeat(jnp.arange(token_count, dtype=jnp.int32), TOPK)
    table = jnp.full((EXPERTS * per_expert,), token_count, jnp.int32).at[slots].set(token_ids)
    padded = jnp.concatenate([route_normed, jnp.zeros((1, route_normed.shape[1]), route_normed.dtype)], axis=0)

    def expert(pieces):
        index, gate_w, up_w, down_w = pieces
        picked_rows = padded[index]
        gate_part = jnp.dot(picked_rows, gate_w, preferred_element_type=jnp.float32)
        up_part = jnp.dot(picked_rows, up_w, preferred_element_type=jnp.float32)
        hidden = (jax.nn.silu(gate_part) * up_part).astype(jnp.bfloat16)
        return group_sum(hidden, down_w, N_TP)
    results = lax.map(expert, (table.reshape(EXPERTS, per_expert), w_gate_e, w_up_e, w_down_e))
    chosen = results.reshape(EXPERTS * per_expert, -1)[slots].reshape(token_count, TOPK, -1).astype(jnp.float32)
    route_out = lax.optimization_barrier(jnp.sum(route_weight[:, :, None] * chosen, axis=1)).astype(jnp.bfloat16)
    return (mixer_out, route_out)
```

```python
import functools

import jax
import jax.numpy as jnp
from jax import lax
from jax.experimental import pallas as pl
from jax.experimental.pallas import tpu as pltpu
from jax.sharding import Mesh
from jax.sharding import PartitionSpec as P

HD = 128
BLK = 256
QROWS = 128
CAPQ = 16
EP = ("ep_0", "ep_1", "ep_2")
EP_TP = ("ep_0", "ep_1", "ep_2", "tp")
EPS = 1e-06
NEG = -1e30
HIGH = lax.Precision.HIGHEST
F32 = jnp.float32
BF16 = jnp.bfloat16
MESH = pl.DeviceIdType.MESH
SROWS = 136


def vmem(count):
    return [pl.BlockSpec(memory_space=pltpu.VMEM)] * count


def iota(shape, dim):
    return lax.broadcasted_iota(jnp.int32, shape, dim)


def dot(left, right, dims=((1,), (0,)), precision=None):
    return lax.dot_general(
        left, right, (dims, ((), ())), precision=precision, preferred_element_type=F32
    )


def normed_rows(rows, gain):
    wide = rows.astype(F32)
    scale = lax.rsqrt(jnp.mean(wide * wide, axis=-1, keepdims=True) + EPS)
    return (wide * scale * gain).astype(BF16)


def join(earlier, later):
    memory_a, normer_a, stable_a, total_a = earlier
    memory_b, normer_b, stable_b, total_b = later
    stable = jnp.maximum(total_b + stable_a, stable_b)
    scale_a = jnp.exp(total_b + stable_a - stable)
    scale_b = jnp.exp(stable_b - stable)
    return (
        scale_a * memory_a + scale_b * memory_b,
        scale_a * normer_a + scale_b * normer_b,
        stable,
        total_a + total_b,
    )


def load_state(ref, at):
    tail = ref[(*at, slice(128, SROWS), slice(None))]
    return (ref[(*at, slice(0, 128), slice(None))], tail[0:1], tail[1:2], tail[2:3])


def store_state(ref, at, state):
    memory, normer, stable, total = state
    ref[(*at, slice(0, 128), slice(None))] = memory
    ref[(*at, slice(128, SROWS), slice(None))] = jnp.concatenate(
        [normer, stable, total, jnp.zeros((SROWS - 131, 128), F32)], axis=0
    )


def empty_state(stable):
    return (
        jnp.zeros((128, 128), F32),
        jnp.zeros((1, 128), F32),
        jnp.full((1, 128), stable, F32),
        jnp.zeros((1, 128), F32),
    )


def pick(test, new, old):
    return tuple(jnp.where(test, a, b) for a, b in zip(new, old))


def scan_lanes(rows, op, identity, reverse):
    width = rows.shape[1]
    lane = iota(rows.shape, 1)
    step = 1
    while step < width:
        if reverse:
            moved = jnp.where(lane < width - step, pltpu.roll(rows, width - step, 1), identity)
        else:
            moved = jnp.where(lane >= step, pltpu.roll(rows, step, 1), identity)
        rows = op(rows, moved)
        step *= 2
    return rows


def log_sigmoid(x):
    return jnp.minimum(x, 0.0) - jnp.log1p(jnp.exp(-jnp.abs(x)))


def front_kernel(
    x_ref, gain_ref, wq_ref, wk_ref, wv_ref, wo_ref, wg_ref, bias_ref, drift_ref,
    q_ref, k_ref, v_ref, o_ref, rows_ref, blocks_ref, device_ref,
):
    block = pl.program_id(0)
    turn = lax.rem(8 - 2 * lax.axis_index("tp"), 8)
    normed = normed_rows(x_ref[...], gain_ref[...])
    q_ref[...] = dot(normed, wq_ref[...]).astype(BF16)
    key_rows = (dot(normed, wk_ref[...]) * HD ** (-0.5)).astype(BF16)
    k_ref[...] = key_rows
    value_rows = dot(normed, wv_ref[...]).astype(BF16)
    v_ref[...] = value_rows
    o_ref[...] = dot(normed, wo_ref[...]).astype(BF16)
    gates = dot(normed, wg_ref[...]).T

    def gate(kind):
        return pltpu.roll(gates[8 * kind : 8 * kind + 8], turn, 0)[:2] + bias_ref[kind]

    drift = drift_ref[block, 0]
    run_f = scan_lanes(log_sigmoid(gate(1) + drift), jnp.add, 0.0, False)
    run_b = scan_lanes(log_sigmoid(gate(3) + drift), jnp.add, 0.0, True)
    a_f = gate(0) - run_f
    a_b = gate(2) - run_b
    max_f = scan_lanes(a_f, jnp.maximum, NEG, False)
    max_b = scan_lanes(a_b, jnp.maximum, NEG, True)
    rows_ref[0] = jnp.concatenate(
        [max_f, max_b, run_f, run_b, a_f, a_b, jnp.zeros((4, BLK), F32)], axis=0
    )
    keys_wide = key_rows.astype(F32)
    keys_t = keys_wide.T
    for way, (a_rows, top, total) in enumerate(
        (
            (a_f, max_f[:, BLK - 1 :], run_f[:, BLK - 1 :]),
            (a_b, max_b[:, :1], run_b[:, :1]),
        )
    ):
        weights = jnp.exp(a_rows - top)
        normers = dot(weights, keys_wide, precision=HIGH)
        for head in range(2):
            at = slice(head * HD, (head + 1) * HD)
            weighted = (keys_t[at] * weights[head : head + 1]).astype(BF16)
            here = (
                dot(weighted, value_rows[:, at]),
                normers[head : head + 1, at],
                jnp.broadcast_to((total + top)[head : head + 1], (1, 128)),
                jnp.broadcast_to(total[head : head + 1], (1, 128)),
            )
            store_state(blocks_ref, (0, way, head), here)

            @pl.when(block == 0)
            def _():
                store_state(device_ref, (way, head), here)

            @pl.when(block > 0)
            def _():
                so_far = load_state(device_ref, (way, head))
                both = join(so_far, here) if way == 0 else join(here, so_far)
                store_state(device_ref, (way, head), both)


def mixer_front(x, gain, wq, wk, wv, wo, wg, bias, drift):
    rows = x.shape[0]
    count = rows // BLK
    wide = wq.shape[1]
    whole = lambda shape: pl.BlockSpec(shape, lambda b: (0,) * len(shape))
    by_rows = lambda width: pl.BlockSpec((BLK, width), lambda b: (b, 0))
    return pl.pallas_call(
        front_kernel,
        grid=(count,),
        out_shape=[jax.ShapeDtypeStruct((rows, wide), BF16)] * 4
        + [
            jax.ShapeDtypeStruct((count, 16, BLK), F32),
            jax.ShapeDtypeStruct((count, 2, 2, SROWS, 128), F32),
            jax.ShapeDtypeStruct((2, 2, SROWS, 128), F32),
        ],
        in_specs=[
            by_rows(x.shape[1]),
            whole(gain.shape),
            whole(wq.shape),
            whole(wk.shape),
            whole(wv.shape),
            whole(wo.shape),
            whole(wg.shape),
            whole(bias.shape),
            pl.BlockSpec(memory_space=pltpu.SMEM),
        ],
        out_specs=[by_rows(wide)] * 4
        + [
            pl.BlockSpec((1, 16, BLK), lambda b: (b, 0, 0)),
            pl.BlockSpec((1, 2, 2, SROWS, 128), lambda b: (b, 0, 0, 0, 0)),
            whole((2, 2, SROWS, 128)),
        ],
        cost_estimate=pl.CostEstimate(
            flops=2 * rows * x.shape[1] * (4 * wide + 32), bytes_accessed=12 << 20, transcendentals=0
        ),
        name="mixer_front",
    )(x, gain, wq, wk, wv, wo, wg, bias, drift)


def exchange_kernel(own_ref, out_ref, partner, ys, zs, back, send_sem, recv_sem):
    z, y, c = (lax.axis_index(name) for name in EP)
    ny, nz = lax.axis_size("ep_1"), lax.axis_size("ep_0")
    other = {"ep_2": 1 - c}

    barrier = pltpu.get_barrier_semaphore()
    peers = [other]
    peers += [{"ep_1": lax.rem(y + d, ny)} for d in range(1, ny)]
    peers += [{"ep_0": lax.rem(z + d, nz)} for d in range(1, nz)]
    for peer in peers:
        pl.semaphore_signal(barrier, inc=1, device_id=peer, device_id_type=MESH)
    pl.semaphore_wait(barrier, len(peers))

    def remote(number, src, dst, peer):
        copy = pltpu.make_async_remote_copy(
            src_ref=src,
            dst_ref=dst,
            send_sem=send_sem.at[number],
            recv_sem=recv_sem.at[number],
            device_id=peer,
            device_id_type=MESH,
        )
        copy.start()
        return copy

    swap = remote(0, own_ref.at[1 - c], partner, other)
    swap.wait_recv()
    pos_y = jnp.where(c == 0, y, ny - 1 - y)
    pos_z = jnp.where(c == 0, z, nz - 1 - z)
    for head in range(2):
        store_state(
            ys, (pos_y, head), join(load_state(own_ref, (c, head)), load_state(partner, (head,)))
        )
    sent = [swap]
    hops = [
        remote(d, ys.at[pos_y], ys.at[pos_y], {"ep_1": lax.rem(y + d, ny)}) for d in range(1, ny)
    ]
    for copy in hops:
        copy.wait_recv()
    sent += hops
    inside = []
    for head in range(2):
        subtotal = load_state(ys, (0, head))
        before = pick(0 < pos_y, subtotal, empty_state(NEG))
        for k in range(1, ny):
            subtotal = join(subtotal, load_state(ys, (k, head)))
            before = pick(k < pos_y, subtotal, before)
        store_state(zs, (pos_z, head), subtotal)
        store_state(back, (0, head), before)
    hops = [
        remote(ny - 1 + d, zs.at[pos_z], zs.at[pos_z], {"ep_0": lax.rem(z + d, nz)})
        for d in range(1, nz)
    ]
    for copy in hops:
        copy.wait_recv()
    sent += hops
    for head in range(2):
        chain = before = empty_state(0.0)
        for k in range(nz - 1):
            chain = join(chain, load_state(zs, (k, head)))
            before = pick(k < pos_z, chain, before)
        entering = join(before, load_state(back, (0, head)))
        store_state(out_ref, (c, head), entering)
        store_state(back, (1, head), join(entering, load_state(own_ref, (c, head))))
    last = remote(ny + nz - 1, back.at[1], back.at[2], other)
    last.wait_recv()
    for head in range(2):
        store_state(out_ref, (1 - c, head), load_state(back, (2, head)))
    for copy in sent + [last]:
        copy.wait_send()


def exchange_states(own):
    ny, nz = lax.axis_size("ep_1"), lax.axis_size("ep_0")
    copies = ny + nz
    return pl.pallas_call(
        exchange_kernel,
        out_shape=jax.ShapeDtypeStruct(own.shape, F32),
        in_specs=vmem(1),
        out_specs=pl.BlockSpec(memory_space=pltpu.VMEM),
        scratch_shapes=[
            pltpu.VMEM((2, SROWS, 128), F32),
            pltpu.VMEM((ny, 2, SROWS, 128), F32),
            pltpu.VMEM((nz, 2, SROWS, 128), F32),
            pltpu.VMEM((3, 2, SROWS, 128), F32),
            pltpu.SemaphoreType.DMA((copies,)),
            pltpu.SemaphoreType.DMA((copies,)),
        ],
        compiler_params=pltpu.CompilerParams(collective_id=1, has_side_effects=True),
        cost_estimate=pl.CostEstimate(flops=10 << 27, bytes_accessed=1 << 20, transcendentals=0),
        name="exchange_states",
    )(own)


def heads_kernel(
    q_ref, k_ref, v_ref, o_ref, rows_ref, blocks_ref, enter_ref, gain_ref, out_ref, mem_ref, norm_ref
):
    count = blocks_ref.shape[0]
    own = lax.axis_index("tp")
    for head in range(2):
        cols = slice(0, 128), slice(128, 256)
        for way in range(2):
            state = load_state(enter_ref, (way, head))
            for step in range(count):
                b = step if way == 0 else count - 1 - step
                mem_ref[b, head, :, cols[way]] = state[0].astype(BF16)
                norm_ref[b, head, 4 * way : 4 * way + 4, :] = jnp.concatenate(
                    [state[1], state[2], state[2], state[2]], axis=0
                )
                if step < count - 1:
                    state = join(state, load_state(blocks_ref, (b, way, head)))
    tri = iota((BLK, BLK), 0) >= iota((BLK, BLK), 1)

    def one_block(b, carry):
        at_rows = pl.ds(pl.multiple_of(b * BLK, BLK), BLK)
        rows = rows_ref[b]
        cols = rows.T
        place = jnp.bitwise_xor(b, own)
        for head in range(2):
            at = slice(head * HD, (head + 1) * HD)
            col = lambda kind: cols[:, 2 * kind + head : 2 * kind + head + 1]
            row = lambda kind: rows[2 * kind + head : 2 * kind + head + 1]
            query, keys, values = q_ref[at_rows, at], k_ref[at_rows, at], v_ref[at_rows, at]
            tails = norm_ref[b, head]
            in_f, in_b = tails[1:2, :1], tails[5:6, :1]
            top_f = jnp.maximum(col(0), in_f)
            top_b = jnp.maximum(col(1), in_b)
            raw = dot(query, keys, ((1,), (1,)))
            scores = raw * jnp.exp(jnp.where(tri, row(4) - top_f, row(5) - top_b))
            query_wide = query.astype(F32)
            carried = dot(query, mem_ref[b, head])
            into_f = jnp.exp(in_f - top_f)
            into_b = jnp.exp(in_b - top_b)
            sum_f = jnp.sum(jnp.where(tri, scores, 0.0), axis=1, keepdims=True)
            sum_b = jnp.sum(jnp.where(tri, 0.0, scores), axis=1, keepdims=True)
            carried_f = jnp.sum(query_wide * tails[0:1], axis=1, keepdims=True)
            carried_b = jnp.sum(query_wide * tails[4:5], axis=1, keepdims=True)
            itself = jnp.sum(query_wide * keys.astype(F32), axis=1, keepdims=True) * jnp.exp(
                col(5) - top_b
            )
            under_f = jnp.abs(sum_f + into_f * carried_f)
            under_b = jnp.abs(sum_b + itself + into_b * carried_b)
            part_f = 1.0 / jnp.maximum(under_f, jnp.exp(-(col(2) + top_f)))
            part_b = 1.0 / jnp.maximum(under_b, jnp.exp(-(col(3) + top_b)))
            mixed = dot((scores * jnp.where(tri, part_f, part_b)).astype(BF16), values)
            mixed += (itself * part_b) * values.astype(F32)
            mixed += (into_f * part_f) * carried[:, :128] + (into_b * part_b) * carried[:, 128:]
            gated = jax.nn.sigmoid(o_ref[at_rows, at].astype(F32)) * mixed
            out_ref[place, :, at] = normed_rows(gated, gain_ref[:, at])
        return carry

    lax.fori_loop(0, count, one_block, 0)


def mixer_heads(q, k, v, o, rows, blocks, enter, gain):
    count = blocks.shape[0]
    return pl.pallas_call(
        heads_kernel,
        out_shape=jax.ShapeDtypeStruct((count, BLK, q.shape[1]), BF16),
        in_specs=vmem(8),
        out_specs=pl.BlockSpec(memory_space=pltpu.VMEM),
        scratch_shapes=[
            pltpu.VMEM((count, 2, 128, 256), BF16),
            pltpu.VMEM((count, 2, 8, 128), F32),
        ],
        cost_estimate=pl.CostEstimate(flops=5 << 29, bytes_accessed=4 << 20, transcendentals=0),
        name="mixer_heads",
    )(q, k, v, o, rows, blocks, enter, gain)


def sum_kernel(count, *refs):
    total = dot(refs[0][...], refs[count][...])
    for k in range(1, count):
        total += dot(refs[k][...], refs[count + k][...])
    refs[-1][...] = total.astype(BF16)


def sum_of_products(lefts, rights, tile, name):
    rows, wide = lefts[0].shape[0], rights[0].shape[1]
    count = len(lefts)
    return pl.pallas_call(
        functools.partial(sum_kernel, count),
        grid=(wide // tile,),
        out_shape=jax.ShapeDtypeStruct((rows, wide), BF16),
        in_specs=[pl.BlockSpec(a.shape, lambda n: (0, 0)) for a in lefts]
        + [pl.BlockSpec((b.shape[0], tile), lambda n: (0, n)) for b in rights],
        out_specs=pl.BlockSpec((rows, tile), lambda n: (0, n)),
        cost_estimate=pl.CostEstimate(
            flops=2 * rows * wide * sum(a.shape[1] for a in lefts),
            bytes_accessed=8 << 20,
            transcendentals=0,
        ),
        name=name,
    )(*lefts, *rights)


def slot_keys(pair, experts):
    named = ((pair[0:1] == experts) | (pair[1:2] == experts)).astype(F32)
    earlier = (iota((QROWS, QROWS), 0) < iota((QROWS, QROWS), 1)).astype(BF16)
    return jnp.where(named > 0, dot(named.astype(BF16), earlier), -1.0)


def slot_onehot(pair, experts):
    keys = slot_keys(pair, experts)
    places = iota((keys.shape[0], CAPQ, QROWS), 1).astype(F32)
    hot = (jnp.broadcast_to(keys[:, None, :], places.shape) == places).astype(F32)
    return hot.reshape(keys.shape[0] * CAPQ, QROWS)


def dispatch_kernel(x_ref, gain_ref, routes_ref, out_ref):
    own = lax.axis_index("tp")
    experts = out_ref.shape[0] * 2
    width = x_ref.shape[1]
    half = experts // 2
    for kind, partner in enumerate((0, 3, 1)):
        number = jnp.bitwise_xor(own, partner)
        start = pl.ds(pl.multiple_of(number * QROWS, QROWS), QROWS)
        rows = normed_rows(x_ref[start, :], gain_ref[...])
        pair = routes_ref[:, start]
        for core in range(2):
            if kind == 2 - core:
                continue
            ids = 2 * iota((half, QROWS), 0) + core
            hot = slot_onehot(pair, ids).astype(BF16)
            picked = dot(hot, rows).astype(BF16).reshape(half, CAPQ, width)
            out_ref[:, core, min(kind, 1)] = picked


def dispatch(x, gain, routes_t, experts):
    return pl.pallas_call(
        dispatch_kernel,
        out_shape=jax.ShapeDtypeStruct((experts // 2, 2, 2, CAPQ, x.shape[1]), BF16),
        in_specs=vmem(3),
        out_specs=pl.BlockSpec(memory_space=pltpu.VMEM),
        cost_estimate=pl.CostEstimate(flops=1 << 29, bytes_accessed=6 << 20, transcendentals=0),
        name="dispatch",
    )(x, gain, routes_t)


def hidden_kernel(x_ref, ga_ref, gb_ref, ua_ref, ub_ref, own_ref, other_ref):
    sources, _, cap, width = x_ref.shape
    for block, out_ref in enumerate((own_ref, other_ref)):
        rows = x_ref[:, block].reshape(sources * cap, width)
        for part, (gate, up) in enumerate(((ga_ref, ua_ref), (gb_ref, ub_ref))):
            gate_part = dot(rows, gate[...])
            up_part = dot(rows, up[...])
            wide = gate.shape[1]
            out_ref[:, part * wide : (part + 1) * wide] = (
                jax.nn.silu(gate_part) * up_part
            ).astype(BF16)


def expert_hidden(arrived, gate_a, gate_b, up_a, up_b):
    sources, _, cap, width = arrived.shape
    rows, wide = sources * cap, 2 * gate_a.shape[1]
    step = 8
    weight = pl.BlockSpec(gate_a.shape, lambda s: (0, 0))
    out = pl.BlockSpec((step * cap, wide), lambda s: (s, 0))
    return pl.pallas_call(
        hidden_kernel,
        grid=(sources // step,),
        out_shape=[jax.ShapeDtypeStruct((rows, wide), BF16)] * 2,
        in_specs=[pl.BlockSpec((step, 2, cap, width), lambda s: (s, 0, 0, 0))] + [weight] * 4,
        out_specs=[out, out],
        cost_estimate=pl.CostEstimate(
            flops=8 * rows * wide * width, bytes_accessed=9 << 20, transcendentals=0
        ),
        name="expert_hidden",
    )(arrived, gate_a, gate_b, up_a, up_b)


def combine_kernel(rows_ref, routes_ref, weight_ref, out_ref):
    experts = rows_ref.shape[0] // CAPQ
    own = lax.axis_index("tp")
    pair = routes_ref[:, pl.ds(pl.multiple_of(own * QROWS, QROWS), QROWS)]
    ids = iota((experts, QROWS), 0)
    weight = jnp.where(pair[0:1] == ids, weight_ref[0:1], 0.0) + jnp.where(
        pair[1:2] == ids, weight_ref[1:2], 0.0
    )
    spread = jnp.broadcast_to(weight[:, None, :], (experts, CAPQ, QROWS)).reshape(-1, QROWS)
    factor = (slot_onehot(pair, ids) * spread).T
    high = factor.astype(BF16)
    low = (factor - high.astype(F32)).astype(BF16)
    rows = rows_ref[...]
    out_ref[...] = (dot(high, rows) + dot(low, rows)).astype(BF16)


def combine(returned, routes_t, weight_t):
    return pl.pallas_call(
        combine_kernel,
        out_shape=jax.ShapeDtypeStruct((QROWS, returned.shape[1]), BF16),
        in_specs=vmem(3),
        out_specs=pl.BlockSpec(memory_space=pltpu.VMEM),
        cost_estimate=pl.CostEstimate(flops=1 << 29, bytes_accessed=3 << 20, transcendentals=0),
        name="combine",
    )(returned, routes_t, weight_t)


def shards(
    x_mix, mix_gain, w_query, w_key, w_value, w_outgate, w_gates, gate_bias, gate_drift, head_gain,
    w_out, x_route, route_gain, routes, route_weight, w_gate_e, w_up_e, w_down_e,
):
    groups = lax.axis_size("tp")
    experts = lax.axis_size(EP)

    def swap(value, first, second):
        pairs = [(k, k ^ first) for k in range(groups)]
        pairs += [(groups + k, groups + (k ^ second)) for k in range(groups)]
        return lax.ppermute(value, ("ep_2", "tp"), pairs)

    routes_t = routes.T
    weight_t = route_weight.T
    outgoing = dispatch(x_route, route_gain[None], routes_t, experts)
    outgoing = outgoing.reshape(experts, 2, CAPQ, -1)
    arrived = lax.all_to_all(outgoing, EP, split_axis=0, concat_axis=0, tiled=True)
    gate_w, up_w, down_w = w_gate_e[0], w_up_e[0], w_down_e[0]
    gate_b = swap(gate_w, 1, 3)
    up_b = swap(up_w, 1, 3)
    downs = [down_w, swap(down_w, 1, 3), swap(down_w, 3, 1), swap(down_w, 2, 2)]
    outs = [w_out] + [swap(w_out, k, k) for k in (1, 2, 3)]

    q, k, v, o, rows, blocks, own_state = mixer_front(
        x_mix, mix_gain[None], w_query, w_key, w_value, w_outgate, w_gates, gate_bias[:, :, None],
        gate_drift[:, None],
    )
    enter = exchange_states(own_state)
    heads = mixer_heads(q, k, v, o, rows, blocks, enter, head_gain[None])
    mine = [heads[0]] + [swap(heads[k], k, k) for k in (1, 2, 3)]

    hidden, hidden_other = expert_hidden(arrived, gate_w, gate_b, up_w, up_b)
    hidden_more = swap(hidden_other, 3, 1)
    wide = down_w.shape[0]
    results = sum_of_products(
        [hidden[:, :wide], hidden[:, wide:], hidden_more[:, :wide], hidden_more[:, wide:]],
        downs, 512, "expert_out",
    )
    returned = lax.all_to_all(
        results.reshape(experts, CAPQ, -1), EP, split_axis=0, concat_axis=0, tiled=True
    )
    mixer_out = sum_of_products(mine, outs, 512, "mixer_out")
    route_out = combine(returned.reshape(experts * CAPQ, -1), routes_t, weight_t)
    return (mixer_out, route_out)


def solution(mesh):
    finer = Mesh(mesh.devices.reshape(4, 4, 2, mesh.shape["tp"]), ("ep_0", "ep_1", "ep_2", "tp"))
    in_specs = (
        P(EP, None), P(), P(None, "tp"), P(None, "tp"), P(None, "tp"), P(None, "tp"), P(),
        P(None, "tp"), P(EP), P("tp"), P("tp", None), P(EP, None), P(), P(EP, None),
        P(EP_TP, None), P(EP, None, "tp"), P(EP, None, "tp"), P(EP, "tp", None),
    )
    out_specs = (P(EP_TP, None), P(EP_TP, None))
    return jax.shard_map(
        shards, mesh=finer, in_specs=in_specs, out_specs=out_specs, check_vma=False
    )
```

```python
import functools

import jax
import jax.numpy as jnp
from jax import lax
from jax.experimental import pallas as pl
from jax.experimental.pallas import tpu as pltpu
from jax.sharding import Mesh
from jax.sharding import PartitionSpec as P

HD = 128
BLK = 256
QROWS = 128
CAPQ = 16
EP = ("ep_0", "ep_1", "ep_2")
EP_TP = ("ep_0", "ep_1", "ep_2", "tp")
EPS = 1e-06
NEG = -1e30
HIGH = lax.Precision.HIGHEST
F32 = jnp.float32
BF16 = jnp.bfloat16
MESH = pl.DeviceIdType.MESH
SROWS = 136


def vmem(count):
    return [pl.BlockSpec(memory_space=pltpu.VMEM)] * count


def iota(shape, dim):
    return lax.broadcasted_iota(jnp.int32, shape, dim)


def dot(left, right, dims=((1,), (0,)), precision=None):
    return lax.dot_general(
        left, right, (dims, ((), ())), precision=precision, preferred_element_type=F32
    )


def normed_rows(rows, gain):
    wide = rows.astype(F32)
    scale = lax.rsqrt(jnp.mean(wide * wide, axis=-1, keepdims=True) + EPS)
    return (wide * scale * gain).astype(BF16)


def join(earlier, later):
    memory_a, normer_a, stable_a, total_a = earlier
    memory_b, normer_b, stable_b, total_b = later
    stable = jnp.maximum(total_b + stable_a, stable_b)
    scale_a = jnp.exp(total_b + stable_a - stable)
    scale_b = jnp.exp(stable_b - stable)
    return (
        scale_a * memory_a + scale_b * memory_b,
        scale_a * normer_a + scale_b * normer_b,
        stable,
        total_a + total_b,
    )


def load_state(ref, at):
    tail = ref[(*at, slice(128, SROWS), slice(None))]
    return (ref[(*at, slice(0, 128), slice(None))], tail[0:1], tail[1:2], tail[2:3])


def store_state(ref, at, state):
    memory, normer, stable, total = state
    ref[(*at, slice(0, 128), slice(None))] = memory
    ref[(*at, slice(128, SROWS), slice(None))] = jnp.concatenate(
        [normer, stable, total, jnp.zeros((SROWS - 131, 128), F32)], axis=0
    )


def empty_state(stable):
    return (
        jnp.zeros((128, 128), F32),
        jnp.zeros((1, 128), F32),
        jnp.full((1, 128), stable, F32),
        jnp.zeros((1, 128), F32),
    )


def pick(test, new, old):
    return tuple(jnp.where(test, a, b) for a, b in zip(new, old))


def scan_lanes(rows, op, identity, reverse):
    width = rows.shape[1]
    lane = iota(rows.shape, 1)
    step = 1
    while step < width:
        if reverse:
            moved = jnp.where(lane < width - step, pltpu.roll(rows, width - step, 1), identity)
        else:
            moved = jnp.where(lane >= step, pltpu.roll(rows, step, 1), identity)
        rows = op(rows, moved)
        step *= 2
    return rows


def log_sigmoid(x):
    return jnp.minimum(x, 0.0) - jnp.log1p(jnp.exp(-jnp.abs(x)))


def front_kernel(
    x_ref, gain_ref, wq_ref, wk_ref, wv_ref, wo_ref, wg_ref, bias_ref, drift_ref,
    q_ref, k_ref, v_ref, o_ref, rows_ref, blocks_ref, device_ref,
):
    block = pl.program_id(0)
    turn = lax.rem(8 - 2 * lax.axis_index("tp"), 8)
    normed = normed_rows(x_ref[...], gain_ref[...])
    q_ref[...] = dot(normed, wq_ref[...]).astype(BF16)
    key_rows = (dot(normed, wk_ref[...]) * HD ** (-0.5)).astype(BF16)
    k_ref[...] = key_rows
    value_rows = dot(normed, wv_ref[...]).astype(BF16)
    v_ref[...] = value_rows
    o_ref[...] = dot(normed, wo_ref[...]).astype(BF16)
    gates = dot(normed, wg_ref[...]).T

    def gate(kind):
        return pltpu.roll(gates[8 * kind : 8 * kind + 8], turn, 0)[:2] + bias_ref[kind]

    drift = drift_ref[block, 0]
    run_f = scan_lanes(log_sigmoid(gate(1) + drift), jnp.add, 0.0, False)
    run_b = scan_lanes(log_sigmoid(gate(3) + drift), jnp.add, 0.0, True)
    a_f = gate(0) - run_f
    a_b = gate(2) - run_b
    max_f = scan_lanes(a_f, jnp.maximum, NEG, False)
    max_b = scan_lanes(a_b, jnp.maximum, NEG, True)
    rows_ref[0] = jnp.concatenate(
        [max_f, max_b, run_f, run_b, a_f, a_b, jnp.zeros((4, BLK), F32)], axis=0
    )
    keys_wide = key_rows.astype(F32)
    keys_t = keys_wide.T
    for way, (a_rows, top, total) in enumerate(
        (
            (a_f, max_f[:, BLK - 1 :], run_f[:, BLK - 1 :]),
            (a_b, max_b[:, :1], run_b[:, :1]),
        )
    ):
        weights = jnp.exp(a_rows - top)
        normers = dot(weights, keys_wide, precision=HIGH)
        for head in range(2):
            at = slice(head * HD, (head + 1) * HD)
            weighted = (keys_t[at] * weights[head : head + 1]).astype(BF16)
            here = (
                dot(weighted, value_rows[:, at]),
                normers[head : head + 1, at],
                jnp.broadcast_to((total + top)[head : head + 1], (1, 128)),
                jnp.broadcast_to(total[head : head + 1], (1, 128)),
            )
            store_state(blocks_ref, (0, way, head), here)

            @pl.when(block == 0)
            def _():
                store_state(device_ref, (way, head), here)

            @pl.when(block > 0)
            def _():
                so_far = load_state(device_ref, (way, head))
                both = join(so_far, here) if way == 0 else join(here, so_far)
                store_state(device_ref, (way, head), both)


def mixer_front(x, gain, wq, wk, wv, wo, wg, bias, drift):
    rows = x.shape[0]
    count = rows // BLK
    wide = wq.shape[1]
    whole = lambda shape: pl.BlockSpec(shape, lambda b: (0,) * len(shape))
    by_rows = lambda width: pl.BlockSpec((BLK, width), lambda b: (b, 0))
    return pl.pallas_call(
        front_kernel,
        grid=(count,),
        out_shape=[jax.ShapeDtypeStruct((rows, wide), BF16)] * 4
        + [
            jax.ShapeDtypeStruct((count, 16, BLK), F32),
            jax.ShapeDtypeStruct((count, 2, 2, SROWS, 128), F32),
            jax.ShapeDtypeStruct((2, 2, SROWS, 128), F32),
        ],
        in_specs=[
            by_rows(x.shape[1]),
            whole(gain.shape),
            whole(wq.shape),
            whole(wk.shape),
            whole(wv.shape),
            whole(wo.shape),
            whole(wg.shape),
            whole(bias.shape),
            pl.BlockSpec(memory_space=pltpu.SMEM),
        ],
        out_specs=[by_rows(wide)] * 4
        + [
            pl.BlockSpec((1, 16, BLK), lambda b: (b, 0, 0)),
            pl.BlockSpec((1, 2, 2, SROWS, 128), lambda b: (b, 0, 0, 0, 0)),
            whole((2, 2, SROWS, 128)),
        ],
        cost_estimate=pl.CostEstimate(
            flops=2 * rows * x.shape[1] * (4 * wide + 32), bytes_accessed=12 << 20, transcendentals=0
        ),
        name="mixer_front",
    )(x, gain, wq, wk, wv, wo, wg, bias, drift)


def exchange_kernel(own_ref, out_ref, partner, ys, zs, back, send_sem, recv_sem):
    z, y, c = (lax.axis_index(name) for name in EP)
    ny, nz = lax.axis_size("ep_1"), lax.axis_size("ep_0")
    other = {"ep_2": 1 - c}

    barrier = pltpu.get_barrier_semaphore()
    peers = [other]
    peers += [{"ep_1": lax.rem(y + d, ny)} for d in range(1, ny)]
    peers += [{"ep_0": lax.rem(z + d, nz)} for d in range(1, nz)]
    for peer in peers:
        pl.semaphore_signal(barrier, inc=1, device_id=peer, device_id_type=MESH)
    pl.semaphore_wait(barrier, len(peers))

    def remote(number, src, dst, peer):
        copy = pltpu.make_async_remote_copy(
            src_ref=src,
            dst_ref=dst,
            send_sem=send_sem.at[number],
            recv_sem=recv_sem.at[number],
            device_id=peer,
            device_id_type=MESH,
        )
        copy.start()
        return copy

    swap = remote(0, own_ref.at[1 - c], partner, other)
    swap.wait_recv()
    pos_y = jnp.where(c == 0, y, ny - 1 - y)
    pos_z = jnp.where(c == 0, z, nz - 1 - z)
    for head in range(2):
        store_state(
            ys, (pos_y, head), join(load_state(own_ref, (c, head)), load_state(partner, (head,)))
        )
    sent = [swap]
    hops = [
        remote(d, ys.at[pos_y], ys.at[pos_y], {"ep_1": lax.rem(y + d, ny)}) for d in range(1, ny)
    ]
    for copy in hops:
        copy.wait_recv()
    sent += hops
    inside = []
    for head in range(2):
        subtotal = load_state(ys, (0, head))
        before = pick(0 < pos_y, subtotal, empty_state(NEG))
        for k in range(1, ny):
            subtotal = join(subtotal, load_state(ys, (k, head)))
            before = pick(k < pos_y, subtotal, before)
        store_state(zs, (pos_z, head), subtotal)
        store_state(back, (0, head), before)
    hops = [
        remote(ny - 1 + d, zs.at[pos_z], zs.at[pos_z], {"ep_0": lax.rem(z + d, nz)})
        for d in range(1, nz)
    ]
    for copy in hops:
        copy.wait_recv()
    sent += hops
    for head in range(2):
        chain = before = empty_state(0.0)
        for k in range(nz - 1):
            chain = join(chain, load_state(zs, (k, head)))
            before = pick(k < pos_z, chain, before)
        entering = join(before, load_state(back, (0, head)))
        store_state(out_ref, (c, head), entering)
        store_state(back, (1, head), join(entering, load_state(own_ref, (c, head))))
    last = remote(ny + nz - 1, back.at[1], back.at[2], other)
    last.wait_recv()
    for head in range(2):
        store_state(out_ref, (1 - c, head), load_state(back, (2, head)))
    for copy in sent + [last]:
        copy.wait_send()


def exchange_states(own):
    ny, nz = lax.axis_size("ep_1"), lax.axis_size("ep_0")
    copies = ny + nz
    return pl.pallas_call(
        exchange_kernel,
        out_shape=jax.ShapeDtypeStruct(own.shape, F32),
        in_specs=vmem(1),
        out_specs=pl.BlockSpec(memory_space=pltpu.VMEM),
        scratch_shapes=[
            pltpu.VMEM((2, SROWS, 128), F32),
            pltpu.VMEM((ny, 2, SROWS, 128), F32),
            pltpu.VMEM((nz, 2, SROWS, 128), F32),
            pltpu.VMEM((3, 2, SROWS, 128), F32),
            pltpu.SemaphoreType.DMA((copies,)),
            pltpu.SemaphoreType.DMA((copies,)),
        ],
        compiler_params=pltpu.CompilerParams(collective_id=1, has_side_effects=True),
        cost_estimate=pl.CostEstimate(flops=10 << 27, bytes_accessed=1 << 20, transcendentals=0),
        name="exchange_states",
    )(own)


def heads_kernel(
    q_ref, k_ref, v_ref, o_ref, rows_ref, blocks_ref, enter_ref, gain_ref, out_ref, mem_ref, norm_ref
):
    count = blocks_ref.shape[0]
    own = lax.axis_index("tp")
    for head in range(2):
        cols = slice(0, 128), slice(128, 256)
        for way in range(2):
            state = load_state(enter_ref, (way, head))
            for step in range(count):
                b = step if way == 0 else count - 1 - step
                mem_ref[b, head, :, cols[way]] = state[0].astype(BF16)
                norm_ref[b, head, 4 * way : 4 * way + 4, :] = jnp.concatenate(
                    [state[1], state[2], state[2], state[2]], axis=0
                )
                if step < count - 1:
                    state = join(state, load_state(blocks_ref, (b, way, head)))
    tri = iota((BLK, BLK), 0) >= iota((BLK, BLK), 1)

    def one_block(b, carry):
        at_rows = pl.ds(pl.multiple_of(b * BLK, BLK), BLK)
        rows = rows_ref[b]
        cols = rows.T
        place = jnp.bitwise_xor(b, own)
        for head in range(2):
            at = slice(head * HD, (head + 1) * HD)
            col = lambda kind: cols[:, 2 * kind + head : 2 * kind + head + 1]
            row = lambda kind: rows[2 * kind + head : 2 * kind + head + 1]
            query, keys, values = q_ref[at_rows, at], k_ref[at_rows, at], v_ref[at_rows, at]
            tails = norm_ref[b, head]
            in_f, in_b = tails[1:2, :1], tails[5:6, :1]
            top_f = jnp.maximum(col(0), in_f)
            top_b = jnp.maximum(col(1), in_b)
            raw = dot(query, keys, ((1,), (1,)))
            scores = raw * jnp.exp(jnp.where(tri, row(4) - top_f, row(5) - top_b))
            query_wide = query.astype(F32)
            carried = dot(query, mem_ref[b, head])
            into_f = jnp.exp(in_f - top_f)
            into_b = jnp.exp(in_b - top_b)
            sum_f = jnp.sum(jnp.where(tri, scores, 0.0), axis=1, keepdims=True)
            sum_b = jnp.sum(jnp.where(tri, 0.0, scores), axis=1, keepdims=True)
            carried_f = jnp.sum(query_wide * tails[0:1], axis=1, keepdims=True)
            carried_b = jnp.sum(query_wide * tails[4:5], axis=1, keepdims=True)
            itself = jnp.sum(query_wide * keys.astype(F32), axis=1, keepdims=True) * jnp.exp(
                col(5) - top_b
            )
            under_f = jnp.abs(sum_f + into_f * carried_f)
            under_b = jnp.abs(sum_b + itself + into_b * carried_b)
            part_f = 1.0 / jnp.maximum(under_f, jnp.exp(-(col(2) + top_f)))
            part_b = 1.0 / jnp.maximum(under_b, jnp.exp(-(col(3) + top_b)))
            mixed = dot((scores * jnp.where(tri, part_f, part_b)).astype(BF16), values)
            mixed += (itself * part_b) * values.astype(F32)
            mixed += (into_f * part_f) * carried[:, :128] + (into_b * part_b) * carried[:, 128:]
            gated = jax.nn.sigmoid(o_ref[at_rows, at].astype(F32)) * mixed
            out_ref[place, :, at] = normed_rows(gated, gain_ref[:, at])
        return carry

    lax.fori_loop(0, count, one_block, 0)


def mixer_heads(q, k, v, o, rows, blocks, enter, gain):
    count = blocks.shape[0]
    return pl.pallas_call(
        heads_kernel,
        out_shape=jax.ShapeDtypeStruct((count, BLK, q.shape[1]), BF16),
        in_specs=vmem(8),
        out_specs=pl.BlockSpec(memory_space=pltpu.VMEM),
        scratch_shapes=[
            pltpu.VMEM((count, 2, 128, 256), BF16),
            pltpu.VMEM((count, 2, 8, 128), F32),
        ],
        cost_estimate=pl.CostEstimate(flops=5 << 29, bytes_accessed=4 << 20, transcendentals=0),
        name="mixer_heads",
    )(q, k, v, o, rows, blocks, enter, gain)


def sum_kernel(count, *refs):
    total = dot(refs[0][...], refs[count][...])
    for k in range(1, count):
        total += dot(refs[k][...], refs[count + k][...])
    refs[-1][...] = total.astype(BF16)


def sum_of_products(lefts, rights, tile, name):
    rows, wide = lefts[0].shape[0], rights[0].shape[1]
    count = len(lefts)
    return pl.pallas_call(
        functools.partial(sum_kernel, count),
        grid=(wide // tile,),
        out_shape=jax.ShapeDtypeStruct((rows, wide), BF16),
        in_specs=[pl.BlockSpec(a.shape, lambda n: (0, 0)) for a in lefts]
        + [pl.BlockSpec((b.shape[0], tile), lambda n: (0, n)) for b in rights],
        out_specs=pl.BlockSpec((rows, tile), lambda n: (0, n)),
        cost_estimate=pl.CostEstimate(
            flops=2 * rows * wide * sum(a.shape[1] for a in lefts),
            bytes_accessed=8 << 20,
            transcendentals=0,
        ),
        name=name,
    )(*lefts, *rights)


def slot_keys(pair, experts):
    named = ((pair[0:1] == experts) | (pair[1:2] == experts)).astype(F32)
    earlier = (iota((QROWS, QROWS), 0) < iota((QROWS, QROWS), 1)).astype(BF16)
    return jnp.where(named > 0, dot(named.astype(BF16), earlier), -1.0)


def slot_onehot(pair, experts):
    keys = slot_keys(pair, experts)
    places = iota((keys.shape[0], CAPQ, QROWS), 1).astype(F32)
    hot = (jnp.broadcast_to(keys[:, None, :], places.shape) == places).astype(F32)
    return hot.reshape(keys.shape[0] * CAPQ, QROWS)


def dispatch_kernel(x_ref, gain_ref, routes_ref, out_ref):
    own = lax.axis_index("tp")
    experts = out_ref.shape[0] * 2
    width = x_ref.shape[1]
    half = experts // 2
    for kind, partner in enumerate((0, 3, 1)):
        number = jnp.bitwise_xor(own, partner)
        start = pl.ds(pl.multiple_of(number * QROWS, QROWS), QROWS)
        rows = normed_rows(x_ref[start, :], gain_ref[...])
        pair = routes_ref[:, start]
        for core in range(2):
            if kind == 2 - core:
                continue
            ids = 2 * iota((half, QROWS), 0) + core
            hot = slot_onehot(pair, ids).astype(BF16)
            picked = dot(hot, rows).astype(BF16).reshape(half, CAPQ, width)
            out_ref[:, core, min(kind, 1)] = picked


def dispatch(x, gain, routes_t, experts):
    return pl.pallas_call(
        dispatch_kernel,
        out_shape=jax.ShapeDtypeStruct((experts // 2, 2, 2, CAPQ, x.shape[1]), BF16),
        in_specs=vmem(3),
        out_specs=pl.BlockSpec(memory_space=pltpu.VMEM),
        cost_estimate=pl.CostEstimate(flops=1 << 29, bytes_accessed=6 << 20, transcendentals=0),
        name="dispatch",
    )(x, gain, routes_t)


def hidden_kernel(x_ref, ga_ref, gb_ref, ua_ref, ub_ref, own_ref, other_ref):
    sources, _, cap, width = x_ref.shape
    for block, out_ref in enumerate((own_ref, other_ref)):
        rows = x_ref[:, block].reshape(sources * cap, width)
        for part, (gate, up) in enumerate(((ga_ref, ua_ref), (gb_ref, ub_ref))):
            gate_part = dot(rows, gate[...])
            up_part = dot(rows, up[...])
            wide = gate.shape[1]
            out_ref[:, part * wide : (part + 1) * wide] = (
                jax.nn.silu(gate_part) * up_part
            ).astype(BF16)


def expert_hidden(arrived, gate_a, gate_b, up_a, up_b):
    sources, _, cap, width = arrived.shape
    rows, wide = sources * cap, 2 * gate_a.shape[1]
    step = 8
    weight = pl.BlockSpec(gate_a.shape, lambda s: (0, 0))
    out = pl.BlockSpec((step * cap, wide), lambda s: (s, 0))
    return pl.pallas_call(
        hidden_kernel,
        grid=(sources // step,),
        out_shape=[jax.ShapeDtypeStruct((rows, wide), BF16)] * 2,
        in_specs=[pl.BlockSpec((step, 2, cap, width), lambda s: (s, 0, 0, 0))] + [weight] * 4,
        out_specs=[out, out],
        cost_estimate=pl.CostEstimate(
            flops=8 * rows * wide * width, bytes_accessed=9 << 20, transcendentals=0
        ),
        name="expert_hidden",
    )(arrived, gate_a, gate_b, up_a, up_b)


def combine_kernel(rows_ref, routes_ref, weight_ref, out_ref):
    experts = rows_ref.shape[0] // CAPQ
    own = lax.axis_index("tp")
    pair = routes_ref[:, pl.ds(pl.multiple_of(own * QROWS, QROWS), QROWS)]
    ids = iota((experts, QROWS), 0)
    weight = jnp.where(pair[0:1] == ids, weight_ref[0:1], 0.0) + jnp.where(
        pair[1:2] == ids, weight_ref[1:2], 0.0
    )
    spread = jnp.broadcast_to(weight[:, None, :], (experts, CAPQ, QROWS)).reshape(-1, QROWS)
    factor = (slot_onehot(pair, ids) * spread).T
    high = factor.astype(BF16)
    low = (factor - high.astype(F32)).astype(BF16)
    rows = rows_ref[...]
    out_ref[...] = (dot(high, rows) + dot(low, rows)).astype(BF16)


def combine(returned, routes_t, weight_t):
    return pl.pallas_call(
        combine_kernel,
        out_shape=jax.ShapeDtypeStruct((QROWS, returned.shape[1]), BF16),
        in_specs=vmem(3),
        out_specs=pl.BlockSpec(memory_space=pltpu.VMEM),
        cost_estimate=pl.CostEstimate(flops=1 << 29, bytes_accessed=3 << 20, transcendentals=0),
        name="combine",
    )(returned, routes_t, weight_t)


def shards(
    x_mix, mix_gain, w_query, w_key, w_value, w_outgate, w_gates, gate_bias, gate_drift, head_gain,
    w_out, x_route, route_gain, routes, route_weight, w_gate_e, w_up_e, w_down_e,
):
    groups = lax.axis_size("tp")
    experts = lax.axis_size(EP)

    def swap(value, first, second):
        pairs = [(k, k ^ first) for k in range(groups)]
        pairs += [(groups + k, groups + (k ^ second)) for k in range(groups)]
        return lax.ppermute(value, ("ep_2", "tp"), pairs)

    routes_t = routes.T
    weight_t = route_weight.T
    outgoing = dispatch(x_route, route_gain[None], routes_t, experts)
    outgoing = outgoing.reshape(experts, 2, CAPQ, -1)
    arrived = lax.all_to_all(outgoing, EP, split_axis=0, concat_axis=0, tiled=True)
    gate_w, up_w, down_w = w_gate_e[0], w_up_e[0], w_down_e[0]
    gate_b = swap(gate_w, 1, 3)
    up_b = swap(up_w, 1, 3)
    downs = [down_w, swap(down_w, 1, 3), swap(down_w, 3, 1), swap(down_w, 2, 2)]
    outs = [w_out] + [swap(w_out, k, k) for k in (1, 2, 3)]

    q, k, v, o, rows, blocks, own_state = mixer_front(
        x_mix, mix_gain[None], w_query, w_key, w_value, w_outgate, w_gates, gate_bias[:, :, None],
        gate_drift[:, None],
    )
    enter = exchange_states(own_state)
    arrived, enter = lax.optimization_barrier((arrived, enter))
    hidden, hidden_other = expert_hidden(arrived, gate_w, gate_b, up_w, up_b)
    hidden_more = swap(hidden_other, 3, 1)
    wide = down_w.shape[0]
    results = sum_of_products(
        [hidden[:, :wide], hidden[:, wide:], hidden_more[:, :wide], hidden_more[:, wide:]],
        downs, 512, "expert_out",
    )
    returned = lax.all_to_all(
        results.reshape(experts, CAPQ, -1), EP, split_axis=0, concat_axis=0, tiled=True
    )
    heads = mixer_heads(q, k, v, o, rows, blocks, enter, head_gain[None])
    mine = [heads[0]] + [swap(heads[k], k, k) for k in (1, 2, 3)]

    mixer_out = sum_of_products(mine, outs, 512, "mixer_out")
    route_out = combine(returned.reshape(experts * CAPQ, -1), routes_t, weight_t)
    return (mixer_out, route_out)


def solution(mesh):
    finer = Mesh(mesh.devices.reshape(4, 4, 2, mesh.shape["tp"]), ("ep_0", "ep_1", "ep_2", "tp"))
    in_specs = (
        P(EP, None), P(), P(None, "tp"), P(None, "tp"), P(None, "tp"), P(None, "tp"), P(),
        P(None, "tp"), P(EP), P("tp"), P("tp", None), P(EP, None), P(), P(EP, None),
        P(EP_TP, None), P(EP, None, "tp"), P(EP, None, "tp"), P(EP, "tp", None),
    )
    out_specs = (P(EP_TP, None), P(EP_TP, None))
    return jax.shard_map(
        shards, mesh=finer, in_specs=in_specs, out_specs=out_specs, check_vma=False
    )
```
